32 devices in a mesh: rep: 4 (over z), fs: 4 (over y, x), tp: 2 (over core).
Axes of the slice: x: 2, y: 2, z: 4, core: 2. Of those that a mesh axis runs over, the one named last changes fastest.
Arguments:
- inputs: bfloat16 [512, 2048], P(('rep', 'fs', 'tp')), may hold values from -6 to 6
- cotangent: bfloat16 [512, 2048], P(('rep', 'fs', 'tp')), may hold values from -6 to 6
- norm_gain: float32 [2048], replicated, may hold values from 0.1 to 1.9
- gate_weight: bfloat16 [2048, 2816], P(None, ('fs', 'tp')), may hold values from -0.125 to 0.125
- up_weight: bfloat16 [2048, 2816], P(None, ('fs', 'tp')), may hold values from -0.125 to 0.125
- down_weight: bfloat16 [2816, 2048], P(('fs', 'tp')), may hold values from -0.109375 to 0.109375
Outputs:
- input_grad: bfloat16 [512, 2048], P(('rep', 'fs', 'tp'))
- gain_grad: float32 [2048], replicated
- down_grad: float32 [2816, 2048], P(('fs', 'tp'), 'rep')
The draws below stay inside these ranges and needn't reach their ends.
All inputs are finite; a program needn't handle non-finite values.
Results may differ from the reference program's by a relative error of at most 0.0066.
Values may be sent and summed in bfloat16 or wider, within the bound.
A program may use at most 64 MiB of HBM per device.

```python
import jax
import jax.numpy as jnp
from jax import lax

D = 2048
FF = 2816
TOKENS = 512


def raised(entries, rng, source, target, shards_of, factor):
    def block_of(axis_at):
        return (jnp.arange(entries.shape[axis_at]) // (entries.shape[axis_at] // shards_of)).reshape((-1,) + (1,) * (entries.ndim - 1 - axis_at))

    near = jax.random.permutation(rng, shards_of)[block_of(target)]
    second = (block_of(target) + shards_of // 2) % shards_of
    return jnp.where((block_of(source) == near) | (block_of(source) == second), factor * entries, entries)


def shard_levels(rng, extent, cuts, smallest, top_value):
    loudness = 1.0
    for axis_at, shards_of in cuts:
        steps = jax.random.uniform(jax.random.fold_in(jax.random.fold_in(rng, 6), axis_at), (shards_of,), jnp.float32, smallest / len(cuts), top_value / len(cuts))
        loudness = loudness * jnp.repeat(jnp.exp(steps), extent[axis_at] // shards_of).reshape((-1,) + (1,) * (len(extent) - 1 - axis_at))
    return loudness


def centred(own_key, extent, deviation, limit, shards=(), kind=jnp.bfloat16):
    values = deviation * jax.random.normal(own_key, extent, jnp.float32)
    if shards:
        values = values * shard_levels(own_key, extent, shards, -0.22, 0.18)
    return jnp.clip(values, -limit, limit).astype(kind)


def heavy_noise(stream_key, shape, scale, reach, pieces, heavy, kind=jnp.bfloat16):
    entries = scale * jax.random.normal(stream_key, shape, jnp.float32)
    if pieces:
        entries = entries * shard_levels(stream_key, shape, pieces, -0.22, 0.18)
    return jnp.clip(raised(entries, jax.random.fold_in(stream_key, 3), *heavy), -reach, reach).astype(kind)


def setup_inputs(seed: int = 0) -> dict:
    streams_of = jax.random.split(jax.random.key(seed), 7)
    return {
        "inputs": centred(streams_of[0], (TOKENS, D), 1.0, 6.0, ((0, 32),)),
        "cotangent": heavy_noise(streams_of[1], (TOKENS, D), 1.0, 6.0, ((0, 32),), (0, 1, 32, 2.75)),
        "norm_gain": jnp.clip(1.0 + 0.18 * jax.random.normal(streams_of[2], (D,), jnp.float32), 0.1, 1.9),
        "gate_weight": centred(streams_of[3], (D, FF), D ** -0.5, 0.125, ((1, 8),)),
        "up_weight": centred(streams_of[4], (D, FF), D ** -0.5, 0.125, ((1, 8),)),
        "down_weight": centred(streams_of[5], (FF, D), FF ** -0.5, 0.109375, ((0, 8),)),
    }


EPS = 1e-06

def reference(inputs, cotangent, norm_gain, gate_weight, up_weight, down_weight):
    xf = inputs.astype(jnp.float32)
    inv = lax.rsqrt(lax.optimization_barrier(jnp.mean(xf * xf, axis=-1, keepdims=True)) + EPS)
    normed = xf * inv
    hidden_in = (normed * norm_gain).astype(jnp.bfloat16)
    gate = jnp.dot(hidden_in, gate_weight, preferred_element_type=jnp.float32)
    up = jnp.dot(hidden_in, up_weight, preferred_element_type=jnp.float32)
    sig = jax.nn.sigmoid(gate)
    act = gate * sig
    hidden = (act * up).astype(jnp.bfloat16)
    d_hidden = 0.5 * jnp.dot(cotangent, down_weight.T, preferred_element_type=jnp.float32)
    d_gate = (d_hidden * up * sig * (1.0 + gate * (1.0 - sig))).astype(jnp.bfloat16)
    d_up = (d_hidden * act).astype(jnp.bfloat16)
    down_grad = 0.5 * jnp.dot(hidden.T, cotangent, preferred_element_type=jnp.float32)
    d_in = jnp.dot(d_gate, gate_weight.T, preferred_element_type=jnp.float32) + jnp.dot(d_up, up_weight.T, preferred_element_type=jnp.float32)
    gain_grad = lax.optimization_barrier(jnp.sum(d_in * normed, axis=0))
    scaled = d_in * norm_gain
    input_grad = (inv * (scaled - normed * lax.optimization_barrier(jnp.mean(scaled * normed, axis=-1, keepdims=True)))).astype(jnp.bfloat16)
    return (input_grad, gain_grad, down_grad)
```

```python
import functools

import jax
import jax.numpy as jnp
from jax import lax
from jax.experimental import pallas as pl
from jax.experimental.pallas import tpu as pltpu
from jax.sharding import PartitionSpec as P

EPS = 1e-06


def across_tokens(left, right):
    return lax.dot_general(
        left, right, (((0,), (0,)), ((), ())), preferred_element_type=jnp.float32
    )


def across_columns(left, right):
    return lax.dot_general(
        left, right, (((1,), (1,)), ((), ())), preferred_element_type=jnp.float32
    )


def per_device(inputs, cotangent, norm_gain, gate_weight, up_weight, down_weight):
    whole_x, whole_dy = (
        lax.all_gather(inputs, ("fs", "tp"), axis=0, tiled=True),
        lax.all_gather(cotangent, ("fs", "tp"), axis=0, tiled=True),
    )
    xf = whole_x.astype(jnp.float32)
    inv = lax.rsqrt(jnp.mean(xf * xf, axis=-1, keepdims=True) + EPS)
    normed = xf * inv
    hidden_in = (normed * norm_gain).astype(jnp.bfloat16)
    gate = jnp.dot(hidden_in, gate_weight, preferred_element_type=jnp.float32)
    up = jnp.dot(hidden_in, up_weight, preferred_element_type=jnp.float32)
    sig = jax.nn.sigmoid(gate)
    act = gate * sig
    hidden = (act * up).astype(jnp.bfloat16)
    d_hidden = 0.5 * across_columns(whole_dy, down_weight)
    d_gate = (d_hidden * up * sig * (1.0 + gate * (1.0 - sig))).astype(jnp.bfloat16)
    d_up = (d_hidden * act).astype(jnp.bfloat16)
    own_rows = inputs.shape[0]
    d_in = lax.psum_scatter(
        across_columns(d_gate, gate_weight) + across_columns(d_up, up_weight),
        ("fs", "tp"),
        scatter_dimension=0,
        tiled=True,
    )
    offset = lax.axis_index(("fs", "tp")) * own_rows
    own_normed = lax.dynamic_slice_in_dim(normed, offset, own_rows, 0)
    own_inv = lax.dynamic_slice_in_dim(inv, offset, own_rows, 0)
    gain_grad = lax.psum(jnp.sum(d_in * own_normed, axis=0), ("rep", "fs", "tp"))
    scaled = d_in * norm_gain
    input_grad = (
        own_inv * (scaled - own_normed * jnp.mean(scaled * own_normed, axis=-1, keepdims=True))
    ).astype(jnp.bfloat16)
    input_grad, gain_grad = (input_grad, gain_grad)
    part_down = 0.5 * across_tokens(whole_dy, hidden)
    got_down = lax.all_to_all(
        part_down[None].astype(jnp.bfloat16), "rep", split_axis=1, concat_axis=0, tiled=True
    ).astype(jnp.float32)
    down_grad = jnp.sum(got_down, axis=0).T
    return (input_grad, gain_grad, down_grad)


MESH = pl.DeviceIdType.MESH
LANES = 128
PIECES = 2


def kernel(
    nr, nf,
    x_ref, dy_ref, gain_ref, wg_hbm, wu_hbm, wd_hbm,
    dx_ref, dgain_ref, ddown_ref,
    wg, wu, wd, xg, dyg, dyc, own_hid, hid, normed, d_in, d_out, d_got, gz_own, gz, gg_own, gg,
    w_sem, x_s, x_r, xs_s, xs_r, y_s, y_r, ys_s, ys_r, cz_s, cz_r, c_s, c_r, cs_s, cs_r,
    h_s, h_r, d_s, d_r, gz_s, gz_r, gg_s, gg_r,
):
    r, f, t = lax.axis_index("rep"), lax.axis_index("fs"), lax.axis_index("tp")
    ng = 2 * nf
    me = 2 * f + t
    own, width = x_ref.shape
    cols = ddown_ref.shape[1]
    sibling = (r, f, 1 - t)

    def chip(k):
        return lax.rem(f + k + nf, nf)

    def layer(k):
        return lax.rem(r + k + nr, nr)

    def member(k):
        g = lax.rem(me + k + ng, ng)
        return g, (r, g // 2, lax.rem(g, 2))

    def rows(g):
        return pl.ds(pl.multiple_of(g * own, own), own)

    def span(p):
        return pl.ds(pl.multiple_of(p * cols, LANES), cols)

    sent = []

    def send(src, dst, ssem, rsem, to):
        copy = pltpu.make_async_remote_copy(
            src_ref=src, dst_ref=dst, send_sem=ssem, recv_sem=rsem,
            device_id=to, device_id_type=MESH,
        )
        copy.start()
        sent.append(copy)

    def arrived(dst, ssem, rsem):
        pltpu.make_async_remote_copy(
            src_ref=dst, dst_ref=dst, send_sem=ssem, recv_sem=rsem,
            device_id=sibling, device_id_type=MESH,
        ).wait_recv()

    loads = [
        pltpu.make_async_copy(src, dst, w_sem.at[i])
        for i, (src, dst) in enumerate(((wg_hbm, wg), (wu_hbm, wu), (wd_hbm, wd)))
    ]
    for load in loads:
        load.start()

    barrier = pltpu.get_barrier_semaphore()
    for k in range(1, ng):
        pl.semaphore_signal(barrier, inc=1, device_id=member(k)[1], device_id_type=MESH)
    for k in range(1, nr):
        pl.semaphore_signal(barrier, inc=1, device_id=(layer(k), f, t), device_id_type=MESH)
    pl.semaphore_wait(barrier, ng - 1 + nr - 1)

    for src, dst, ss, rs, bs, br in (
        (x_ref, xg, x_s, x_r, xs_s, xs_r), (dy_ref, dyg, y_s, y_r, ys_s, ys_r)
    ):
        for k in range(1, nf):
            send(src, dst.at[rows(me)], ss.at[k - 1], rs.at[k - 1], (r, chip(k), t))
        send(src, dst.at[rows(me)], bs.at[0], br.at[0], sibling)
    for k in range(1, nr):
        to = layer(k)
        send(
            dy_ref.at[:, span(to)], dyc.at[k - 1, rows(me)],
            cz_s.at[k - 1], cz_r.at[k - 1], (to, f, t),
        )
    xg[rows(me), :] = x_ref[...]
    dyg[rows(me), :] = dy_ref[...]

    def hand_on(ref, at, ss, rs, bs, br):
        for k in range(1, nf):
            block = at(ref, 2 * chip(-k) + t)
            arrived(block, ss.at[k - 1], rs.at[k - 1])
            send(block, block, bs.at[k], br.at[k], sibling)

    def from_sibling(ref, at, bs, br):
        for k in range(nf):
            arrived(at(ref, 2 * chip(-k) + 1 - t), bs.at[k], br.at[k])

    def plain(ref, g):
        return ref.at[rows(g)]

    def stacked(ref, g):
        return ref.at[:, rows(g)]

    hand_on(xg, plain, x_s, x_r, xs_s, xs_r)
    from_sibling(xg, plain, xs_s, xs_r)

    xf = xg[...].astype(jnp.float32)
    inv = lax.rsqrt(jnp.mean(xf * xf, axis=-1, keepdims=True) + EPS)
    normed[...] = xf * inv
    hidden_in = (normed[...] * gain_ref[...]).astype(jnp.bfloat16)
    for load in loads:
        load.wait()
    gate = jnp.dot(hidden_in, wg[...], preferred_element_type=jnp.float32)
    up = jnp.dot(hidden_in, wu[...], preferred_element_type=jnp.float32)

    hand_on(dyg, plain, y_s, y_r, ys_s, ys_r)
    for k in range(1, nr):
        arrived(dyc.at[k - 1, rows(me)], cz_s.at[k - 1], cz_r.at[k - 1])
    for k in range(1, nf):
        send(stacked(dyc, me), stacked(dyc, me), c_s.at[k - 1], c_r.at[k - 1], (r, chip(k), t))
    send(stacked(dyc, me), stacked(dyc, me), cs_s.at[0], cs_r.at[0], sibling)
    sig = jax.nn.sigmoid(gate)
    act = gate * sig
    own_hid[...] = (act * up).astype(jnp.bfloat16)
    for k in range(1, nr):
        send(own_hid, hid.at[k - 1], h_s.at[k - 1], h_r.at[k - 1], (layer(k), f, t))

    from_sibling(dyg, plain, ys_s, ys_r)
    d_hidden = 0.5 * across_columns(dyg[...], wd[...])
    d_gate = (d_hidden * up * sig * (1.0 + gate * (1.0 - sig))).astype(jnp.bfloat16)
    d_up = (d_hidden * act).astype(jnp.bfloat16)

    step = width // PIECES
    for p in range(PIECES):
        part = slice(p * step, (p + 1) * step)
        d_in[:, part] = across_columns(d_gate, wg[part, :]) + across_columns(d_up, wu[part, :])
        d_out[:, part] = d_in[:, part].astype(jnp.bfloat16)
        gz_own[:, part] = jnp.sum(d_in[:, part] * normed[:, part], axis=0, keepdims=True)
        for k in range(1, ng):
            g, to = member(k)
            send(
                d_out.at[rows(g), part], d_got.at[k - 1, :, part],
                d_s.at[p, k - 1], d_r.at[p, k - 1], to,
            )
    for k in range(1, nr):
        send(gz_own, gz.at[r], gz_s.at[k - 1], gz_r.at[k - 1], (layer(k), f, t))
    gz[r] = gz_own[...]

    hand_on(dyc, stacked, c_s, c_r, cs_s, cs_r)
    total = across_tokens(own_hid[...], dyg[:, span(r)])

    for k in range(1, nr):
        arrived(gz.at[layer(-k)], gz_s.at[k - 1], gz_r.at[k - 1])
    gg_own[...] = jnp.sum(gz[...], axis=0)
    for k in range(1, ng):
        send(gg_own, gg.at[me], gg_s.at[k - 1], gg_r.at[k - 1], member(k)[1])
    gg[me] = gg_own[...]

    from_sibling(dyc, stacked, cs_s, cs_r)
    for k in range(1, nr):
        arrived(hid.at[k - 1], h_s.at[k - 1], h_r.at[k - 1])
        total = total + across_tokens(hid[k - 1], dyc[k - 1])
    ddown_ref[...] = 0.5 * total

    mine = d_in[rows(me), :]
    for k in range(1, ng):
        for p in range(PIECES):
            arrived(
                d_got.at[k - 1, :, slice(p * step, (p + 1) * step)],
                d_s.at[p, k - 1], d_r.at[p, k - 1],
            )
        mine = mine + d_got[k - 1].astype(jnp.float32)
    xf = x_ref[...].astype(jnp.float32)
    own_inv = lax.rsqrt(jnp.mean(xf * xf, axis=-1, keepdims=True) + EPS)
    own_normed = xf * own_inv
    scaled = mine * gain_ref[...]
    dx_ref[...] = (
        own_inv * (scaled - own_normed * jnp.mean(scaled * own_normed, axis=-1, keepdims=True))
    ).astype(jnp.bfloat16)

    for k in range(1, ng):
        arrived(gg.at[member(-k)[0]], gg_s.at[k - 1], gg_r.at[k - 1])
    dgain_ref[...] = jnp.sum(gg[...], axis=0)
    for copy in sent:
        copy.wait_send()


def fused(nr, nf, inputs, cotangent, norm_gain, gate_weight, up_weight, down_weight):
    own, width = inputs.shape
    share = gate_weight.shape[1]
    ng = 2 * nf
    group, cols = ng * own, width // nr
    bf16, f32 = jnp.bfloat16, jnp.float32
    vmem = pl.BlockSpec(memory_space=pltpu.VMEM)
    hbm = pl.BlockSpec(memory_space=pl.ANY)
    dma = pltpu.SemaphoreType.DMA
    pair = lambda *n: [dma(n), dma(n)]
    dx, dgain, ddown = pl.pallas_call(
        functools.partial(kernel, nr, nf),
        out_shape=(
            jax.ShapeDtypeStruct((own, width), bf16),
            jax.ShapeDtypeStruct((1, width), f32),
            jax.ShapeDtypeStruct((share, cols), f32),
        ),
        in_specs=[vmem] * 3 + [hbm] * 3,
        out_specs=(vmem,) * 3,
        scratch_shapes=[
            pltpu.VMEM((width, share), bf16),
            pltpu.VMEM((width, share), bf16),
            pltpu.VMEM((share, width), bf16),
            pltpu.VMEM((group, width), bf16),
            pltpu.VMEM((group, width), bf16),
            pltpu.VMEM((nr - 1, group, cols), bf16),
            pltpu.VMEM((group, share), bf16),
            pltpu.VMEM((nr - 1, group, share), bf16),
            pltpu.VMEM((group, width), f32),
            pltpu.VMEM((group, width), f32),
            pltpu.VMEM((group, width), bf16),
            pltpu.VMEM((ng - 1, own, width), bf16),
            pltpu.VMEM((1, width), f32),
            pltpu.VMEM((nr, 1, width), f32),
            pltpu.VMEM((1, width), f32),
            pltpu.VMEM((ng, 1, width), f32),
            dma((3,)),
        ]
        + pair(nf - 1) + pair(nf) + pair(nf - 1) + pair(nf)
        + pair(nr - 1) + pair(nf - 1) + pair(nf)
        + pair(nr - 1) + pair(PIECES, ng - 1) + pair(nr - 1) + pair(ng - 1),
        compiler_params=pltpu.CompilerParams(
            collective_id=0, has_side_effects=True, vmem_limit_bytes=48 * 1024 * 1024
        ),
    )(inputs, cotangent, norm_gain[None], gate_weight, up_weight, down_weight)
    return dx, dgain[0], ddown


def solution(mesh):
    nr, nf, nt = (mesh.shape[name] for name in ("rep", "fs", "tp"))

    def body(inputs, *others):
        block = inputs.shape[1] // nr
        if nt == 2 and nr > 1 and nf > 1 and block % LANES == 0 and inputs.shape[0] % 16 == 0:
            return fused(nr, nf, inputs, *others)
        return per_device(inputs, *others)

    return jax.shard_map(
        body,
        mesh=mesh,
        in_specs=(
            P(("rep", "fs", "tp"), None),
            P(("rep", "fs", "tp"), None),
            P(),
            P(None, ("fs", "tp")),
            P(None, ("fs", "tp")),
            P(("fs", "tp"), None),
        ),
        out_specs=(P(("rep", "fs", "tp"), None), P(), P(("fs", "tp"), "rep")),
        check_vma=False,
    )
```

```python
import functools

import jax
import jax.numpy as jnp
from jax import lax
from jax.experimental import pallas as pl
from jax.experimental.pallas import tpu as pltpu
from jax.sharding import PartitionSpec as P

EPS = 1e-06


def across_tokens(left, right):
    return lax.dot_general(
        left, right, (((0,), (0,)), ((), ())), preferred_element_type=jnp.float32
    )


def across_columns(left, right):
    return lax.dot_general(
        left, right, (((1,), (1,)), ((), ())), preferred_element_type=jnp.float32
    )


def per_device(inputs, cotangent, norm_gain, gate_weight, up_weight, down_weight):
    whole_x, whole_dy = (
        lax.all_gather(inputs, ("fs", "tp"), axis=0, tiled=True),
        lax.all_gather(cotangent, ("fs", "tp"), axis=0, tiled=True),
    )
    xf = whole_x.astype(jnp.float32)
    inv = lax.rsqrt(jnp.mean(xf * xf, axis=-1, keepdims=True) + EPS)
    normed = xf * inv
    hidden_in = (normed * norm_gain).astype(jnp.bfloat16)
    gate = jnp.dot(hidden_in, gate_weight, preferred_element_type=jnp.float32)
    up = jnp.dot(hidden_in, up_weight, preferred_element_type=jnp.float32)
    sig = jax.nn.sigmoid(gate)
    act = gate * sig
    hidden = (act * up).astype(jnp.bfloat16)
    d_hidden = 0.5 * across_columns(whole_dy, down_weight)
    d_gate = (d_hidden * up * sig * (1.0 + gate * (1.0 - sig))).astype(jnp.bfloat16)
    d_up = (d_hidden * act).astype(jnp.bfloat16)
    own_rows = inputs.shape[0]
    d_in = lax.psum_scatter(
        across_columns(d_gate, gate_weight) + across_columns(d_up, up_weight),
        ("fs", "tp"),
        scatter_dimension=0,
        tiled=True,
    )
    offset = lax.axis_index(("fs", "tp")) * own_rows
    own_normed = lax.dynamic_slice_in_dim(normed, offset, own_rows, 0)
    own_inv = lax.dynamic_slice_in_dim(inv, offset, own_rows, 0)
    gain_grad = lax.psum(jnp.sum(d_in * own_normed, axis=0), ("rep", "fs", "tp"))
    scaled = d_in * norm_gain
    input_grad = (
        own_inv * (scaled - own_normed * jnp.mean(scaled * own_normed, axis=-1, keepdims=True))
    ).astype(jnp.bfloat16)
    input_grad, gain_grad = (input_grad, gain_grad)
    part_down = 0.5 * across_tokens(whole_dy, hidden)
    got_down = lax.all_to_all(
        part_down[None].astype(jnp.bfloat16), "rep", split_axis=1, concat_axis=0, tiled=True
    ).astype(jnp.float32)
    down_grad = jnp.sum(got_down, axis=0).T
    return (input_grad, gain_grad, down_grad)


MESH = pl.DeviceIdType.MESH
LANES = 128
PIECES = 2


def kernel(
    nr, nf,
    x_ref, dy_ref, gain_ref, wg_hbm, wu_hbm, wd_hbm,
    dx_ref, dgain_ref, ddown_ref,
    wg, wu, wd, xg, dyg, dyc, own_hid, hid, normed, d_in, d_out, d_got, gz_own, gz, gg_own, gg,
    w_sem, x_s, x_r, xs_s, xs_r, y_s, y_r, ys_s, ys_r, cz_s, cz_r, c_s, c_r, cs_s, cs_r,
    h_s, h_r, d_s, d_r, gz_s, gz_r, gg_s, gg_r,
):
    r, f, t = lax.axis_index("rep"), lax.axis_index("fs"), lax.axis_index("tp")
    ng = 2 * nf
    me = 2 * f + t
    own, width = x_ref.shape
    cols = ddown_ref.shape[1]
    sibling = (r, f, 1 - t)

    def chip(k):
        return lax.rem(f + k + nf, nf)

    def layer(k):
        return lax.rem(r + k + nr, nr)

    def member(k):
        g = lax.rem(me + k + ng, ng)
        return g, (r, g // 2, lax.rem(g, 2))

    def rows(g):
        return pl.ds(pl.multiple_of(g * own, own), own)

    def span(p):
        return pl.ds(pl.multiple_of(p * cols, LANES), cols)

    sent = []

    def send(src, dst, ssem, rsem, to):
        copy = pltpu.make_async_remote_copy(
            src_ref=src, dst_ref=dst, send_sem=ssem, recv_sem=rsem,
            device_id=to, device_id_type=MESH,
        )
        copy.start()
        sent.append(copy)

    def arrived(dst, ssem, rsem):
        pltpu.make_async_remote_copy(
            src_ref=dst, dst_ref=dst, send_sem=ssem, recv_sem=rsem,
            device_id=sibling, device_id_type=MESH,
        ).wait_recv()

    loads = [
        pltpu.make_async_copy(src, dst, w_sem.at[i])
        for i, (src, dst) in enumerate(((wg_hbm, wg), (wu_hbm, wu), (wd_hbm, wd)))
    ]
    for load in loads:
        load.start()

    barrier = pltpu.get_barrier_semaphore()
    for k in range(1, ng):
        pl.semaphore_signal(barrier, inc=1, device_id=member(k)[1], device_id_type=MESH)
    for k in range(1, nr):
        pl.semaphore_signal(barrier, inc=1, device_id=(layer(k), f, t), device_id_type=MESH)
    pl.semaphore_wait(barrier, ng - 1 + nr - 1)

    for src, dst, ss, rs, bs, br in (
        (x_ref, xg, x_s, x_r, xs_s, xs_r), (dy_ref, dyg, y_s, y_r, ys_s, ys_r)
    ):
        for k in range(1, nf):
            send(src, dst.at[rows(me)], ss.at[k - 1], rs.at[k - 1], (r, chip(k), t))
        send(src, dst.at[rows(me)], bs.at[0], br.at[0], sibling)
    for k in range(1, nr):
        to = layer(k)
        send(
            dy_ref.at[:, span(to)], dyc.at[k - 1, rows(me)],
            cz_s.at[k - 1], cz_r.at[k - 1], (to, f, t),
        )
    xg[rows(me), :] = x_ref[...]
    dyg[rows(me), :] = dy_ref[...]

    def hand_on(ref, at, ss, rs, bs, br):
        for k in range(1, nf):
            block = at(ref, 2 * chip(-k) + t)
            arrived(block, ss.at[k - 1], rs.at[k - 1])
            send(block, block, bs.at[k], br.at[k], sibling)

    def from_sibling(ref, at, bs, br):
        for k in range(nf):
            arrived(at(ref, 2 * chip(-k) + 1 - t), bs.at[k], br.at[k])

    def plain(ref, g):
        return ref.at[rows(g)]

    def stacked(ref, g):
        return ref.at[:, rows(g)]

    hand_on(xg, plain, x_s, x_r, xs_s, xs_r)
    from_sibling(xg, plain, xs_s, xs_r)

    xf = xg[...].astype(jnp.float32)
    inv = lax.rsqrt(jnp.mean(xf * xf, axis=-1, keepdims=True) + EPS)
    normed[...] = xf * inv
    hidden_in = (normed[...] * gain_ref[...]).astype(jnp.bfloat16)
    for load in loads:
        load.wait()
    gate = across_columns(hidden_in, wg[...])
    up = across_columns(hidden_in, wu[...])

    hand_on(dyg, plain, y_s, y_r, ys_s, ys_r)
    for k in range(1, nr):
        arrived(dyc.at[k - 1, rows(me)], cz_s.at[k - 1], cz_r.at[k - 1])
    for k in range(1, nf):
        send(stacked(dyc, me), stacked(dyc, me), c_s.at[k - 1], c_r.at[k - 1], (r, chip(k), t))
    send(stacked(dyc, me), stacked(dyc, me), cs_s.at[0], cs_r.at[0], sibling)
    sig = jax.nn.sigmoid(gate)
    act = gate * sig
    own_hid[...] = (act * up).astype(jnp.bfloat16)
    for k in range(1, nr):
        send(own_hid, hid.at[k - 1], h_s.at[k - 1], h_r.at[k - 1], (layer(k), f, t))

    from_sibling(dyg, plain, ys_s, ys_r)
    d_hidden = 0.5 * across_columns(dyg[...], wd[...])
    d_gate = (d_hidden * up * sig * (1.0 + gate * (1.0 - sig))).astype(jnp.bfloat16)
    d_up = (d_hidden * act).astype(jnp.bfloat16)

    step = width // PIECES
    for p in range(PIECES):
        part = slice(p * step, (p + 1) * step)
        d_in[:, part] = jnp.dot(
            d_gate, wg[:, part], preferred_element_type=jnp.float32
        ) + jnp.dot(d_up, wu[:, part], preferred_element_type=jnp.float32)
        d_out[:, part] = d_in[:, part].astype(jnp.bfloat16)
        gz_own[:, part] = jnp.sum(d_in[:, part] * normed[:, part], axis=0, keepdims=True)
        for k in range(1, ng):
            g, to = member(k)
            send(
                d_out.at[rows(g), part], d_got.at[k - 1, :, part],
                d_s.at[p, k - 1], d_r.at[p, k - 1], to,
            )
    for k in range(1, nr):
        send(gz_own, gz.at[r], gz_s.at[k - 1], gz_r.at[k - 1], (layer(k), f, t))
    gz[r] = gz_own[...]

    hand_on(dyc, stacked, c_s, c_r, cs_s, cs_r)
    total = across_tokens(own_hid[...], dyg[:, span(r)])

    for k in range(1, nr):
        arrived(gz.at[layer(-k)], gz_s.at[k - 1], gz_r.at[k - 1])
    gg_own[...] = jnp.sum(gz[...], axis=0)
    for k in range(1, ng):
        send(gg_own, gg.at[me], gg_s.at[k - 1], gg_r.at[k - 1], member(k)[1])
    gg[me] = gg_own[...]

    from_sibling(dyc, stacked, cs_s, cs_r)
    for k in range(1, nr):
        arrived(hid.at[k - 1], h_s.at[k - 1], h_r.at[k - 1])
        total = total + across_tokens(hid[k - 1], dyc[k - 1])
    ddown_ref[...] = 0.5 * total

    mine = d_in[rows(me), :]
    for k in range(1, ng):
        for p in range(PIECES):
            arrived(
                d_got.at[k - 1, :, slice(p * step, (p + 1) * step)],
                d_s.at[p, k - 1], d_r.at[p, k - 1],
            )
        mine = mine + d_got[k - 1].astype(jnp.float32)
    xf = x_ref[...].astype(jnp.float32)
    own_inv = lax.rsqrt(jnp.mean(xf * xf, axis=-1, keepdims=True) + EPS)
    own_normed = xf * own_inv
    scaled = mine * gain_ref[...]
    dx_ref[...] = (
        own_inv * (scaled - own_normed * jnp.mean(scaled * own_normed, axis=-1, keepdims=True))
    ).astype(jnp.bfloat16)

    for k in range(1, ng):
        arrived(gg.at[member(-k)[0]], gg_s.at[k - 1], gg_r.at[k - 1])
    dgain_ref[...] = jnp.sum(gg[...], axis=0)
    for copy in sent:
        copy.wait_send()


def fused(nr, nf, inputs, cotangent, norm_gain, gate_weight, up_weight, down_weight):
    own, width = inputs.shape
    share = gate_weight.shape[1]
    ng = 2 * nf
    group, cols = ng * own, width // nr
    bf16, f32 = jnp.bfloat16, jnp.float32
    vmem = pl.BlockSpec(memory_space=pltpu.VMEM)
    hbm = pl.BlockSpec(memory_space=pl.ANY)
    dma = pltpu.SemaphoreType.DMA
    pair = lambda *n: [dma(n), dma(n)]
    dx, dgain, ddown = pl.pallas_call(
        functools.partial(kernel, nr, nf),
        out_shape=(
            jax.ShapeDtypeStruct((own, width), bf16),
            jax.ShapeDtypeStruct((1, width), f32),
            jax.ShapeDtypeStruct((share, cols), f32),
        ),
        in_specs=[vmem] * 3 + [hbm] * 3,
        out_specs=(vmem,) * 3,
        scratch_shapes=[
            pltpu.VMEM((share, width), bf16),
            pltpu.VMEM((share, width), bf16),
            pltpu.VMEM((share, width), bf16),
            pltpu.VMEM((group, width), bf16),
            pltpu.VMEM((group, width), bf16),
            pltpu.VMEM((nr - 1, group, cols), bf16),
            pltpu.VMEM((group, share), bf16),
            pltpu.VMEM((nr - 1, group, share), bf16),
            pltpu.VMEM((group, width), f32),
            pltpu.VMEM((group, width), f32),
            pltpu.VMEM((group, width), bf16),
            pltpu.VMEM((ng - 1, own, width), bf16),
            pltpu.VMEM((1, width), f32),
            pltpu.VMEM((nr, 1, width), f32),
            pltpu.VMEM((1, width), f32),
            pltpu.VMEM((ng, 1, width), f32),
            dma((3,)),
        ]
        + pair(nf - 1) + pair(nf) + pair(nf - 1) + pair(nf)
        + pair(nr - 1) + pair(nf - 1) + pair(nf)
        + pair(nr - 1) + pair(PIECES, ng - 1) + pair(nr - 1) + pair(ng - 1),
        compiler_params=pltpu.CompilerParams(
            collective_id=0, has_side_effects=True
        ),
    )(inputs, cotangent, norm_gain[None], gate_weight.T, up_weight.T, down_weight)
    return dx, dgain[0], ddown


def solution(mesh):
    nr, nf, nt = (mesh.shape[name] for name in ("rep", "fs", "tp"))

    def body(inputs, *others):
        block = inputs.shape[1] // nr
        if nt == 2 and nr > 1 and nf > 1 and block % LANES == 0 and inputs.shape[0] % 16 == 0:
            return fused(nr, nf, inputs, *others)
        return per_device(inputs, *others)

    return jax.shard_map(
        body,
        mesh=mesh,
        in_specs=(
            P(("rep", "fs", "tp"), None),
            P(("rep", "fs", "tp"), None),
            P(),
            P(None, ("fs", "tp")),
            P(None, ("fs", "tp")),
            P(("fs", "tp"), None),
        ),
        out_specs=(P(("rep", "fs", "tp"), None), P(), P(("fs", "tp"), "rep")),
        check_vma=False,
    )
```

```python
import functools

import jax
import jax.numpy as jnp
from jax import lax
from jax.experimental import pallas as pl
from jax.experimental.pallas import tpu as pltpu
from jax.sharding import PartitionSpec as P

EPS = 1e-06


def across_tokens(left, right):
    return lax.dot_general(
        left, right, (((0,), (0,)), ((), ())), preferred_element_type=jnp.float32
    )


def across_columns(left, right):
    return lax.dot_general(
        left, right, (((1,), (1,)), ((), ())), preferred_element_type=jnp.float32
    )


def per_device(inputs, cotangent, norm_gain, gate_weight, up_weight, down_weight):
    whole_x, whole_dy = (
        lax.all_gather(inputs, ("fs", "tp"), axis=0, tiled=True),
        lax.all_gather(cotangent, ("fs", "tp"), axis=0, tiled=True),
    )
    xf = whole_x.astype(jnp.float32)
    inv = lax.rsqrt(jnp.mean(xf * xf, axis=-1, keepdims=True) + EPS)
    normed = xf * inv
    hidden_in = (normed * norm_gain).astype(jnp.bfloat16)
    gate = jnp.dot(hidden_in, gate_weight, preferred_element_type=jnp.float32)
    up = jnp.dot(hidden_in, up_weight, preferred_element_type=jnp.float32)
    sig = jax.nn.sigmoid(gate)
    act = gate * sig
    hidden = (act * up).astype(jnp.bfloat16)
    d_hidden = 0.5 * across_columns(whole_dy, down_weight)
    d_gate = (d_hidden * up * sig * (1.0 + gate * (1.0 - sig))).astype(jnp.bfloat16)
    d_up = (d_hidden * act).astype(jnp.bfloat16)
    own_rows = inputs.shape[0]
    d_in = lax.psum_scatter(
        across_columns(d_gate, gate_weight) + across_columns(d_up, up_weight),
        ("fs", "tp"),
        scatter_dimension=0,
        tiled=True,
    )
    offset = lax.axis_index(("fs", "tp")) * own_rows
    own_normed = lax.dynamic_slice_in_dim(normed, offset, own_rows, 0)
    own_inv = lax.dynamic_slice_in_dim(inv, offset, own_rows, 0)
    gain_grad = lax.psum(jnp.sum(d_in * own_normed, axis=0), ("rep", "fs", "tp"))
    scaled = d_in * norm_gain
    input_grad = (
        own_inv * (scaled - own_normed * jnp.mean(scaled * own_normed, axis=-1, keepdims=True))
    ).astype(jnp.bfloat16)
    input_grad, gain_grad = (input_grad, gain_grad)
    part_down = 0.5 * across_tokens(whole_dy, hidden)
    got_down = lax.all_to_all(
        part_down[None].astype(jnp.bfloat16), "rep", split_axis=1, concat_axis=0, tiled=True
    ).astype(jnp.float32)
    down_grad = jnp.sum(got_down, axis=0).T
    return (input_grad, gain_grad, down_grad)


MESH = pl.DeviceIdType.MESH
LANES = 128
PIECES = 4


def kernel(
    nr, nf,
    x_ref, dy_ref, gain_ref, wg_hbm, wu_hbm, wd_hbm,
    dx_ref, dgain_ref, ddown_ref,
    wg, wu, wd, xg, dyg, dyc, own_hid, hid, normed, d_in, d_out, d_pair, d_send, d_got, gz_own, gz, gg_own, gg,
    w_sem, x_s, x_r, xs_s, xs_r, y_s, y_r, ys_s, ys_r, cz_s, cz_r, c_s, c_r, cs_s, cs_r,
    h_s, h_r, p_s, p_r, d_s, d_r, gz_s, gz_r, gg_s, gg_r,
):
    r, f, t = lax.axis_index("rep"), lax.axis_index("fs"), lax.axis_index("tp")
    ng = 2 * nf
    me = 2 * f + t
    own, width = x_ref.shape
    cols = ddown_ref.shape[1]
    sibling = (r, f, 1 - t)

    def chip(k):
        return lax.rem(f + k + nf, nf)

    def layer(k):
        return lax.rem(r + k + nr, nr)

    def member(k):
        g = lax.rem(me + k + ng, ng)
        return g, (r, g // 2, lax.rem(g, 2))

    def rows(g):
        return pl.ds(pl.multiple_of(g * own, own), own)

    def span(p):
        return pl.ds(pl.multiple_of(p * cols, LANES), cols)

    sent = []

    def send(src, dst, ssem, rsem, to):
        copy = pltpu.make_async_remote_copy(
            src_ref=src, dst_ref=dst, send_sem=ssem, recv_sem=rsem,
            device_id=to, device_id_type=MESH,
        )
        copy.start()
        sent.append(copy)

    def arrived(dst, ssem, rsem):
        pltpu.make_async_remote_copy(
            src_ref=dst, dst_ref=dst, send_sem=ssem, recv_sem=rsem,
            device_id=sibling, device_id_type=MESH,
        ).wait_recv()

    loads = [
        pltpu.make_async_copy(src, dst, w_sem.at[i])
        for i, (src, dst) in enumerate(((wg_hbm, wg), (wu_hbm, wu), (wd_hbm, wd)))
    ]
    for load in loads:
        load.start()

    barrier = pltpu.get_barrier_semaphore()
    for k in range(1, ng):
        pl.semaphore_signal(barrier, inc=1, device_id=member(k)[1], device_id_type=MESH)
    for k in range(1, nr):
        pl.semaphore_signal(barrier, inc=1, device_id=(layer(k), f, t), device_id_type=MESH)
    pl.semaphore_wait(barrier, ng - 1 + nr - 1)

    for src, dst, ss, rs, bs, br in (
        (x_ref, xg, x_s, x_r, xs_s, xs_r), (dy_ref, dyg, y_s, y_r, ys_s, ys_r)
    ):
        for k in range(1, nf):
            send(src, dst.at[rows(me)], ss.at[k - 1], rs.at[k - 1], (r, chip(k), t))
        send(src, dst.at[rows(me)], bs.at[0], br.at[0], sibling)
    for k in range(1, nr):
        to = layer(k)
        send(
            dy_ref.at[:, span(to)], dyc.at[k - 1, rows(me)],
            cz_s.at[k - 1], cz_r.at[k - 1], (to, f, t),
        )
    xg[rows(me), :] = x_ref[...]
    dyg[rows(me), :] = dy_ref[...]

    def hand_on(ref, at, ss, rs, bs, br):
        for k in range(1, nf):
            block = at(ref, 2 * chip(-k) + t)
            arrived(block, ss.at[k - 1], rs.at[k - 1])
            send(block, block, bs.at[k], br.at[k], sibling)

    def from_sibling(ref, at, bs, br):
        for k in range(nf):
            arrived(at(ref, 2 * chip(-k) + 1 - t), bs.at[k], br.at[k])

    def plain(ref, g):
        return ref.at[rows(g)]

    def stacked(ref, g):
        return ref.at[:, rows(g)]

    hand_on(xg, plain, x_s, x_r, xs_s, xs_r)
    from_sibling(xg, plain, xs_s, xs_r)

    xf = xg[...].astype(jnp.float32)
    inv = lax.rsqrt(jnp.mean(xf * xf, axis=-1, keepdims=True) + EPS)
    normed[...] = xf * inv
    hidden_in = (normed[...] * gain_ref[...]).astype(jnp.bfloat16)
    for load in loads:
        load.wait()
    gate = across_columns(hidden_in, wg[...])
    up = across_columns(hidden_in, wu[...])

    sig = jax.nn.sigmoid(gate)
    act = gate * sig
    own_hid[...] = (act * up).astype(jnp.bfloat16)
    for k in range(1, nr):
        send(own_hid, hid.at[k - 1], h_s.at[k - 1], h_r.at[k - 1], (layer(k), f, t))

    hand_on(dyg, plain, y_s, y_r, ys_s, ys_r)
    for k in range(1, nr):
        arrived(dyc.at[k - 1, rows(me)], cz_s.at[k - 1], cz_r.at[k - 1])
    for k in range(1, nf):
        send(stacked(dyc, me), stacked(dyc, me), c_s.at[k - 1], c_r.at[k - 1], (r, chip(k), t))
    send(stacked(dyc, me), stacked(dyc, me), cs_s.at[0], cs_r.at[0], sibling)
    from_sibling(dyg, plain, ys_s, ys_r)
    d_hidden = 0.5 * across_columns(dyg[...], wd[...])
    d_gate = (d_hidden * up * sig * (1.0 + gate * (1.0 - sig))).astype(jnp.bfloat16)
    d_up = (d_hidden * act).astype(jnp.bfloat16)

    step = width // PIECES
    for p in range(PIECES):
        part = slice(p * step, (p + 1) * step)
        d_in[:, part] = jnp.dot(
            d_gate, wg[:, part], preferred_element_type=jnp.float32
        ) + jnp.dot(d_up, wu[:, part], preferred_element_type=jnp.float32)
        d_out[:, :, :, part] = (
            d_in[:, part].astype(jnp.bfloat16).reshape(nf, 2, own, step)
        )
        gg_own[:, part] = jnp.sum(d_in[:, part] * normed[:, part], axis=0, keepdims=True)
        send(
            d_out.at[:, 1 - t, :, part], d_pair.at[:, :, part], p_s.at[p], p_r.at[p], sibling
        )
    for k in range(1, ng):
        send(gg_own, gg.at[me], gg_s.at[k - 1], gg_r.at[k - 1], member(k)[1])
    gg[me] = gg_own[...]

    for p in range(PIECES):
        part = slice(p * step, (p + 1) * step)
        arrived(d_pair.at[:, :, part], p_s.at[p], p_r.at[p])
        for k in range(1, nf):
            to = chip(k)
            d_send[k - 1, :, part] = (
                d_in[rows(2 * to + t), part] + d_pair[to, :, part].astype(jnp.float32)
            ).astype(jnp.bfloat16)
            send(
                d_send.at[k - 1, :, part], d_got.at[k - 1, :, part],
                d_s.at[p, k - 1], d_r.at[p, k - 1], (r, to, t),
            )

    hand_on(dyc, stacked, c_s, c_r, cs_s, cs_r)
    for k in range(1, ng):
        arrived(gg.at[member(-k)[0]], gg_s.at[k - 1], gg_r.at[k - 1])
    gz_own[...] = jnp.sum(gg[...], axis=0)
    for k in range(1, nr):
        send(gz_own, gz.at[r], gz_s.at[k - 1], gz_r.at[k - 1], (layer(k), f, t))
    gz[r] = gz_own[...]
    total = across_tokens(own_hid[...], dyg[:, span(r)])

    from_sibling(dyc, stacked, cs_s, cs_r)
    for k in range(1, nr):
        arrived(hid.at[k - 1], h_s.at[k - 1], h_r.at[k - 1])
        total = total + across_tokens(hid[k - 1], dyc[k - 1])
    ddown_ref[...] = 0.5 * total

    mine = d_in[rows(me), :] + d_pair[f].astype(jnp.float32)
    for k in range(1, nf):
        for p in range(PIECES):
            arrived(
                d_got.at[k - 1, :, slice(p * step, (p + 1) * step)],
                d_s.at[p, k - 1], d_r.at[p, k - 1],
            )
        mine = mine + d_got[k - 1].astype(jnp.float32)
    xf = x_ref[...].astype(jnp.float32)
    own_inv = lax.rsqrt(jnp.mean(xf * xf, axis=-1, keepdims=True) + EPS)
    own_normed = xf * own_inv
    scaled = mine * gain_ref[...]
    dx_ref[...] = (
        own_inv * (scaled - own_normed * jnp.mean(scaled * own_normed, axis=-1, keepdims=True))
    ).astype(jnp.bfloat16)

    for k in range(1, nr):
        arrived(gz.at[layer(-k)], gz_s.at[k - 1], gz_r.at[k - 1])
    dgain_ref[...] = jnp.sum(gz[...], axis=0)
    for copy in sent:
        copy.wait_send()


def put(a, b, c, a_out, b_out, c_out, sem):
    copies = [
        pltpu.make_async_copy(src, dst, sem.at[i])
        for i, (src, dst) in enumerate(((a, a_out), (b, b_out), (c, c_out)))
    ]
    for copy in copies:
        copy.start()
    for copy in copies:
        copy.wait()


def fused(nr, nf, inputs, cotangent, norm_gain, gate_weight, up_weight, down_weight):
    own, width = inputs.shape
    share = gate_weight.shape[1]
    ng = 2 * nf
    group, cols = ng * own, width // nr
    bf16, f32 = jnp.bfloat16, jnp.float32
    vmem = pl.BlockSpec(memory_space=pltpu.VMEM)
    hbm = pl.BlockSpec(memory_space=pltpu.HBM)
    dma = pltpu.SemaphoreType.DMA
    pair = lambda *n: [dma(n), dma(n)]
    results = pl.pallas_call(
        functools.partial(kernel, nr, nf),
        out_shape=(
            jax.ShapeDtypeStruct((own, width), bf16),
            jax.ShapeDtypeStruct((1, width), f32),
            jax.ShapeDtypeStruct((share, cols), f32),
        ),
        in_specs=[vmem] * 3 + [hbm] * 3,
        out_specs=(vmem,) * 3,
        scratch_shapes=[
            pltpu.VMEM((share, width), bf16),
            pltpu.VMEM((share, width), bf16),
            pltpu.VMEM((share, width), bf16),
            pltpu.VMEM((group, width), bf16),
            pltpu.VMEM((group, width), bf16),
            pltpu.VMEM((nr - 1, group, cols), bf16),
            pltpu.VMEM((group, share), bf16),
            pltpu.VMEM((nr - 1, group, share), bf16),
            pltpu.VMEM((group, width), f32),
            pltpu.VMEM((group, width), f32),
            pltpu.VMEM((nf, 2, own, width), bf16),
            pltpu.VMEM((nf, own, width), bf16),
            pltpu.VMEM((nf - 1, own, width), bf16),
            pltpu.VMEM((nf - 1, own, width), bf16),
            pltpu.VMEM((1, width), f32),
            pltpu.VMEM((nr, 1, width), f32),
            pltpu.VMEM((1, width), f32),
            pltpu.VMEM((ng, 1, width), f32),
            dma((3,)),
        ]
        + pair(nf - 1) + pair(nf) + pair(nf - 1) + pair(nf)
        + pair(nr - 1) + pair(nf - 1) + pair(nf)
        + pair(nr - 1) + pair(PIECES) + pair(PIECES, nf - 1) + pair(nr - 1) + pair(ng - 1),
        compiler_params=pltpu.CompilerParams(
            collective_id=0, has_side_effects=True, vmem_limit_bytes=52 * 1024 * 1024
        ),
    )(inputs, cotangent, norm_gain[None], gate_weight.T, up_weight.T, down_weight)
    dx, dgain, ddown = pl.pallas_call(
        put,
        out_shape=tuple(jax.ShapeDtypeStruct(a.shape, a.dtype) for a in results),
        in_specs=[vmem] * 3,
        out_specs=(hbm,) * 3,
        scratch_shapes=[dma((3,))],
        compiler_params=pltpu.CompilerParams(vmem_limit_bytes=52 * 1024 * 1024),
    )(*results)
    return dx, dgain[0], ddown


def solution(mesh):
    nr, nf, nt = (mesh.shape[name] for name in ("rep", "fs", "tp"))

    def body(inputs, *others):
        block = inputs.shape[1] // nr
        if nt == 2 and nr > 1 and nf > 1 and block % LANES == 0 and inputs.shape[0] % 16 == 0:
            return fused(nr, nf, inputs, *others)
        return per_device(inputs, *others)

    return jax.shard_map(
        body,
        mesh=mesh,
        in_specs=(
            P(("rep", "fs", "tp"), None),
            P(("rep", "fs", "tp"), None),
            P(),
            P(None, ("fs", "tp")),
            P(None, ("fs", "tp")),
            P(("fs", "tp"), None),
        ),
        out_specs=(P(("rep", "fs", "tp"), None), P(), P(("fs", "tp"), "rep")),
        check_vma=False,
    )
```

```python
import functools

import jax
import jax.numpy as jnp
from jax import lax
from jax.experimental import pallas as pl
from jax.experimental.pallas import tpu as pltpu
from jax.sharding import PartitionSpec as P

EPS = 1e-06


def across_tokens(left, right):
    return lax.dot_general(
        left, right, (((0,), (0,)), ((), ())), preferred_element_type=jnp.float32
    )


def across_columns(left, right):
    return lax.dot_general(
        left, right, (((1,), (1,)), ((), ())), preferred_element_type=jnp.float32
    )


def per_device(inputs, cotangent, norm_gain, gate_weight, up_weight, down_weight):
    whole_x, whole_dy = (
        lax.all_gather(inputs, ("fs", "tp"), axis=0, tiled=True),
        lax.all_gather(cotangent, ("fs", "tp"), axis=0, tiled=True),
    )
    xf = whole_x.astype(jnp.float32)
    inv = lax.rsqrt(jnp.mean(xf * xf, axis=-1, keepdims=True) + EPS)
    normed = xf * inv
    hidden_in = (normed * norm_gain).astype(jnp.bfloat16)
    gate = jnp.dot(hidden_in, gate_weight, preferred_element_type=jnp.float32)
    up = jnp.dot(hidden_in, up_weight, preferred_element_type=jnp.float32)
    sig = jax.nn.sigmoid(gate)
    act = gate * sig
    hidden = (act * up).astype(jnp.bfloat16)
    d_hidden = 0.5 * across_columns(whole_dy, down_weight)
    d_gate = (d_hidden * up * sig * (1.0 + gate * (1.0 - sig))).astype(jnp.bfloat16)
    d_up = (d_hidden * act).astype(jnp.bfloat16)
    own_rows = inputs.shape[0]
    d_in = lax.psum_scatter(
        across_columns(d_gate, gate_weight) + across_columns(d_up, up_weight),
        ("fs", "tp"),
        scatter_dimension=0,
        tiled=True,
    )
    offset = lax.axis_index(("fs", "tp")) * own_rows
    own_normed = lax.dynamic_slice_in_dim(normed, offset, own_rows, 0)
    own_inv = lax.dynamic_slice_in_dim(inv, offset, own_rows, 0)
    gain_grad = lax.psum(jnp.sum(d_in * own_normed, axis=0), ("rep", "fs", "tp"))
    scaled = d_in * norm_gain
    input_grad = (
        own_inv * (scaled - own_normed * jnp.mean(scaled * own_normed, axis=-1, keepdims=True))
    ).astype(jnp.bfloat16)
    input_grad, gain_grad = (input_grad, gain_grad)
    part_down = 0.5 * across_tokens(whole_dy, hidden)
    got_down = lax.all_to_all(
        part_down[None].astype(jnp.bfloat16), "rep", split_axis=1, concat_axis=0, tiled=True
    ).astype(jnp.float32)
    down_grad = jnp.sum(got_down, axis=0).T
    return (input_grad, gain_grad, down_grad)


MESH = pl.DeviceIdType.MESH
LANES = 128
PIECES = 4


def kernel(
    nr, nf,
    x_hbm, dy_hbm, gain_hbm, wg_hbm, wu_hbm, wd_hbm,
    dx_ref, dgain_ref, ddown_ref,
    x_ref, dy_ref, gain_ref, wg, wu, wd, xg, dyg, dyc, own_hid, hid, normed, d_in, d_out, d_pair, d_send, d_got, gz_own, gz, gg_own, gg,
    w_sem, x_s, x_r, xs_s, xs_r, y_s, y_r, ys_s, ys_r, cz_s, cz_r, c_s, c_r, cs_s, cs_r,
    h_s, h_r, p_s, p_r, d_s, d_r, gz_s, gz_r, gg_s, gg_r,
):
    r, f, t = lax.axis_index("rep"), lax.axis_index("fs"), lax.axis_index("tp")
    ng = 2 * nf
    me = 2 * f + t
    own, width = x_hbm.shape
    cols = ddown_ref.shape[1]
    sibling = (r, f, 1 - t)

    def chip(k):
        return lax.rem(f + k + nf, nf)

    def layer(k):
        return lax.rem(r + k + nr, nr)

    def member(k):
        g = lax.rem(me + k + ng, ng)
        return g, (r, g // 2, lax.rem(g, 2))

    def rows(g):
        return pl.ds(pl.multiple_of(g * own, own), own)

    def span(p):
        return pl.ds(pl.multiple_of(p * cols, LANES), cols)

    sent = []

    def send(src, dst, ssem, rsem, to):
        copy = pltpu.make_async_remote_copy(
            src_ref=src, dst_ref=dst, send_sem=ssem, recv_sem=rsem,
            device_id=to, device_id_type=MESH,
        )
        copy.start()
        sent.append(copy)

    def arrived(dst, ssem, rsem):
        pltpu.make_async_remote_copy(
            src_ref=dst, dst_ref=dst, send_sem=ssem, recv_sem=rsem,
            device_id=sibling, device_id_type=MESH,
        ).wait_recv()

    loads = [
        pltpu.make_async_copy(src, dst, w_sem.at[i])
        for i, (src, dst) in enumerate(
            (
                (x_hbm, x_ref), (dy_hbm, dy_ref), (gain_hbm, gain_ref),
                (wg_hbm, wg), (wu_hbm, wu), (wd_hbm, wd),
            )
        )
    ]
    for load in loads:
        load.start()

    barrier = pltpu.get_barrier_semaphore()
    for k in range(1, ng):
        pl.semaphore_signal(barrier, inc=1, device_id=member(k)[1], device_id_type=MESH)
    for k in range(1, nr):
        pl.semaphore_signal(barrier, inc=1, device_id=(layer(k), f, t), device_id_type=MESH)
    pl.semaphore_wait(barrier, ng - 1 + nr - 1)
    for load in loads[:3]:
        load.wait()

    for src, dst, ss, rs, bs, br in (
        (x_ref, xg, x_s, x_r, xs_s, xs_r), (dy_ref, dyg, y_s, y_r, ys_s, ys_r)
    ):
        for k in range(1, nf):
            send(src, dst.at[rows(me)], ss.at[k - 1], rs.at[k - 1], (r, chip(k), t))
        send(src, dst.at[rows(me)], bs.at[0], br.at[0], sibling)
    for k in range(1, nr):
        to = layer(k)
        send(
            dy_ref.at[:, span(to)], dyc.at[k - 1, rows(me)],
            cz_s.at[k - 1], cz_r.at[k - 1], (to, f, t),
        )
    xg[rows(me), :] = x_ref[...]
    dyg[rows(me), :] = dy_ref[...]

    def hand_on(ref, at, ss, rs, bs, br):
        for k in range(1, nf):
            block = at(ref, 2 * chip(-k) + t)
            arrived(block, ss.at[k - 1], rs.at[k - 1])
            send(block, block, bs.at[k], br.at[k], sibling)

    def from_sibling(ref, at, bs, br):
        for k in range(nf):
            arrived(at(ref, 2 * chip(-k) + 1 - t), bs.at[k], br.at[k])

    def plain(ref, g):
        return ref.at[rows(g)]

    def stacked(ref, g):
        return ref.at[:, rows(g)]

    hand_on(xg, plain, x_s, x_r, xs_s, xs_r)
    from_sibling(xg, plain, xs_s, xs_r)

    xf = xg[...].astype(jnp.float32)
    inv = lax.rsqrt(jnp.mean(xf * xf, axis=-1, keepdims=True) + EPS)
    normed[...] = xf * inv
    hidden_in = (normed[...] * gain_ref[...]).astype(jnp.bfloat16)
    for load in loads[3:]:
        load.wait()
    gate = across_columns(hidden_in, wg[...])
    up = across_columns(hidden_in, wu[...])

    sig = jax.nn.sigmoid(gate)
    act = gate * sig
    own_hid[...] = (act * up).astype(jnp.bfloat16)
    for k in range(1, nr):
        send(own_hid, hid.at[k - 1], h_s.at[k - 1], h_r.at[k - 1], (layer(k), f, t))

    hand_on(dyg, plain, y_s, y_r, ys_s, ys_r)
    for k in range(1, nr):
        arrived(dyc.at[k - 1, rows(me)], cz_s.at[k - 1], cz_r.at[k - 1])
    for k in range(1, nf):
        send(stacked(dyc, me), stacked(dyc, me), c_s.at[k - 1], c_r.at[k - 1], (r, chip(k), t))
    send(stacked(dyc, me), stacked(dyc, me), cs_s.at[0], cs_r.at[0], sibling)
    from_sibling(dyg, plain, ys_s, ys_r)
    d_hidden = 0.5 * across_columns(dyg[...], wd[...])
    d_gate = (d_hidden * up * sig * (1.0 + gate * (1.0 - sig))).astype(jnp.bfloat16)
    d_up = (d_hidden * act).astype(jnp.bfloat16)

    step = width // PIECES
    for p in range(PIECES):
        part = slice(p * step, (p + 1) * step)
        d_in[:, part] = jnp.dot(
            d_gate, wg[:, part], preferred_element_type=jnp.float32
        ) + jnp.dot(d_up, wu[:, part], preferred_element_type=jnp.float32)
        d_out[:, :, :, part] = (
            d_in[:, part].astype(jnp.bfloat16).reshape(nf, 2, own, step)
        )
        gg_own[:, part] = jnp.sum(d_in[:, part] * normed[:, part], axis=0, keepdims=True)
        send(
            d_out.at[:, 1 - t, :, part], d_pair.at[:, :, part], p_s.at[p], p_r.at[p], sibling
        )
    for k in range(1, ng):
        send(gg_own, gg.at[me], gg_s.at[k - 1], gg_r.at[k - 1], member(k)[1])
    gg[me] = gg_own[...]

    for p in range(PIECES):
        part = slice(p * step, (p + 1) * step)
        arrived(d_pair.at[:, :, part], p_s.at[p], p_r.at[p])
        for k in range(1, nf):
            to = chip(k)
            d_send[k - 1, :, part] = (
                d_in[rows(2 * to + t), part] + d_pair[to, :, part].astype(jnp.float32)
            ).astype(jnp.bfloat16)
            send(
                d_send.at[k - 1, :, part], d_got.at[k - 1, :, part],
                d_s.at[p, k - 1], d_r.at[p, k - 1], (r, to, t),
            )

    hand_on(dyc, stacked, c_s, c_r, cs_s, cs_r)
    for k in range(1, ng):
        arrived(gg.at[member(-k)[0]], gg_s.at[k - 1], gg_r.at[k - 1])
    gz_own[...] = jnp.sum(gg[...], axis=0)
    for k in range(1, nr):
        send(gz_own, gz.at[r], gz_s.at[k - 1], gz_r.at[k - 1], (layer(k), f, t))
    gz[r] = gz_own[...]
    total = across_tokens(own_hid[...], dyg[:, span(r)])

    from_sibling(dyc, stacked, cs_s, cs_r)
    for k in range(1, nr):
        arrived(hid.at[k - 1], h_s.at[k - 1], h_r.at[k - 1])
        total = total + across_tokens(hid[k - 1], dyc[k - 1])
    ddown_ref[...] = 0.5 * total

    mine = d_in[rows(me), :] + d_pair[f].astype(jnp.float32)
    for k in range(1, nf):
        for p in range(PIECES):
            arrived(
                d_got.at[k - 1, :, slice(p * step, (p + 1) * step)],
                d_s.at[p, k - 1], d_r.at[p, k - 1],
            )
        mine = mine + d_got[k - 1].astype(jnp.float32)
    xf = x_ref[...].astype(jnp.float32)
    own_inv = lax.rsqrt(jnp.mean(xf * xf, axis=-1, keepdims=True) + EPS)
    own_normed = xf * own_inv
    scaled = mine * gain_ref[...]
    dx_ref[...] = (
        own_inv * (scaled - own_normed * jnp.mean(scaled * own_normed, axis=-1, keepdims=True))
    ).astype(jnp.bfloat16)

    for k in range(1, nr):
        arrived(gz.at[layer(-k)], gz_s.at[k - 1], gz_r.at[k - 1])
    dgain_ref[...] = jnp.sum(gz[...], axis=0)
    for copy in sent:
        copy.wait_send()


def put(a, b, c, a_out, b_out, c_out, sem):
    copies = [
        pltpu.make_async_copy(src, dst, sem.at[i])
        for i, (src, dst) in enumerate(((a, a_out), (b, b_out), (c, c_out)))
    ]
    for copy in copies:
        copy.start()
    for copy in copies:
        copy.wait()


def fused(nr, nf, inputs, cotangent, norm_gain, gate_weight, up_weight, down_weight):
    own, width = inputs.shape
    share = gate_weight.shape[1]
    ng = 2 * nf
    group, cols = ng * own, width // nr
    bf16, f32 = jnp.bfloat16, jnp.float32
    vmem = pl.BlockSpec(memory_space=pltpu.VMEM)
    hbm = pl.BlockSpec(memory_space=pltpu.HBM)
    dma = pltpu.SemaphoreType.DMA
    pair = lambda *n: [dma(n), dma(n)]
    results = pl.pallas_call(
        functools.partial(kernel, nr, nf),
        out_shape=(
            jax.ShapeDtypeStruct((own, width), bf16),
            jax.ShapeDtypeStruct((1, width), f32),
            jax.ShapeDtypeStruct((share, cols), f32),
        ),
        in_specs=[hbm] * 6,
        out_specs=(vmem,) * 3,
        scratch_shapes=[
            pltpu.VMEM((own, width), bf16),
            pltpu.VMEM((own, width), bf16),
            pltpu.VMEM((1, width), f32),
            pltpu.VMEM((share, width), bf16),
            pltpu.VMEM((share, width), bf16),
            pltpu.VMEM((share, width), bf16),
            pltpu.VMEM((group, width), bf16),
            pltpu.VMEM((group, width), bf16),
            pltpu.VMEM((nr - 1, group, cols), bf16),
            pltpu.VMEM((group, share), bf16),
            pltpu.VMEM((nr - 1, group, share), bf16),
            pltpu.VMEM((group, width), f32),
            pltpu.VMEM((group, width), f32),
            pltpu.VMEM((nf, 2, own, width), bf16),
            pltpu.VMEM((nf, own, width), bf16),
            pltpu.VMEM((nf - 1, own, width), bf16),
            pltpu.VMEM((nf - 1, own, width), bf16),
            pltpu.VMEM((1, width), f32),
            pltpu.VMEM((nr, 1, width), f32),
            pltpu.VMEM((1, width), f32),
            pltpu.VMEM((ng, 1, width), f32),
            dma((6,)),
        ]
        + pair(nf - 1) + pair(nf) + pair(nf - 1) + pair(nf)
        + pair(nr - 1) + pair(nf - 1) + pair(nf)
        + pair(nr - 1) + pair(PIECES) + pair(PIECES, nf - 1) + pair(nr - 1) + pair(ng - 1),
        compiler_params=pltpu.CompilerParams(
            collective_id=0, has_side_effects=True, vmem_limit_bytes=52 * 1024 * 1024
        ),
    )(*[
        pltpu.with_memory_space_constraint(a, pltpu.HBM)
        for a in (
            inputs, cotangent, norm_gain[None], gate_weight.T, up_weight.T, down_weight
        )
    ])
    dx, dgain, ddown = pl.pallas_call(
        put,
        out_shape=tuple(jax.ShapeDtypeStruct(a.shape, a.dtype) for a in results),
        in_specs=[vmem] * 3,
        out_specs=(hbm,) * 3,
        scratch_shapes=[dma((3,))],
        compiler_params=pltpu.CompilerParams(vmem_limit_bytes=52 * 1024 * 1024),
    )(*results)
    return dx, dgain[0], ddown


def solution(mesh):
    nr, nf, nt = (mesh.shape[name] for name in ("rep", "fs", "tp"))

    def body(inputs, *others):
        block = inputs.shape[1] // nr
        if nt == 2 and nr > 1 and nf > 1 and block % LANES == 0 and inputs.shape[0] % 16 == 0:
            return fused(nr, nf, inputs, *others)
        return per_device(inputs, *others)

    return jax.shard_map(
        body,
        mesh=mesh,
        in_specs=(
            P(("rep", "fs", "tp"), None),
            P(("rep", "fs", "tp"), None),
            P(),
            P(None, ("fs", "tp")),
            P(None, ("fs", "tp")),
            P(("fs", "tp"), None),
        ),
        out_specs=(P(("rep", "fs", "tp"), None), P(), P(("fs", "tp"), "rep")),
        check_vma=False,
    )
```

```python
import functools

import jax
import jax.numpy as jnp
from jax import lax
from jax.experimental import pallas as pl
from jax.experimental.pallas import tpu as pltpu
from jax.sharding import PartitionSpec as P

EPS = 1e-06


def across_tokens(left, right):
    return lax.dot_general(
        left, right, (((0,), (0,)), ((), ())), preferred_element_type=jnp.float32
    )


def across_columns(left, right):
    return lax.dot_general(
        left, right, (((1,), (1,)), ((), ())), preferred_element_type=jnp.float32
    )


def per_device(inputs, cotangent, norm_gain, gate_weight, up_weight, down_weight):
    whole_x, whole_dy = (
        lax.all_gather(inputs, ("fs", "tp"), axis=0, tiled=True),
        lax.all_gather(cotangent, ("fs", "tp"), axis=0, tiled=True),
    )
    xf = whole_x.astype(jnp.float32)
    inv = lax.rsqrt(jnp.mean(xf * xf, axis=-1, keepdims=True) + EPS)
    normed = xf * inv
    hidden_in = (normed * norm_gain).astype(jnp.bfloat16)
    gate = jnp.dot(hidden_in, gate_weight, preferred_element_type=jnp.float32)
    up = jnp.dot(hidden_in, up_weight, preferred_element_type=jnp.float32)
    sig = jax.nn.sigmoid(gate)
    act = gate * sig
    hidden = (act * up).astype(jnp.bfloat16)
    d_hidden = 0.5 * across_columns(whole_dy, down_weight)
    d_gate = (d_hidden * up * sig * (1.0 + gate * (1.0 - sig))).astype(jnp.bfloat16)
    d_up = (d_hidden * act).astype(jnp.bfloat16)
    own_rows = inputs.shape[0]
    d_in = lax.psum_scatter(
        across_columns(d_gate, gate_weight) + across_columns(d_up, up_weight),
        ("fs", "tp"),
        scatter_dimension=0,
        tiled=True,
    )
    offset = lax.axis_index(("fs", "tp")) * own_rows
    own_normed = lax.dynamic_slice_in_dim(normed, offset, own_rows, 0)
    own_inv = lax.dynamic_slice_in_dim(inv, offset, own_rows, 0)
    gain_grad = lax.psum(jnp.sum(d_in * own_normed, axis=0), ("rep", "fs", "tp"))
    scaled = d_in * norm_gain
    input_grad = (
        own_inv * (scaled - own_normed * jnp.mean(scaled * own_normed, axis=-1, keepdims=True))
    ).astype(jnp.bfloat16)
    input_grad, gain_grad = (input_grad, gain_grad)
    part_down = 0.5 * across_tokens(whole_dy, hidden)
    got_down = lax.all_to_all(
        part_down[None].astype(jnp.bfloat16), "rep", split_axis=1, concat_axis=0, tiled=True
    ).astype(jnp.float32)
    down_grad = jnp.sum(got_down, axis=0).T
    return (input_grad, gain_grad, down_grad)


MESH = pl.DeviceIdType.MESH
LANES = 128
PIECES = 4


def kernel(
    nr, nf,
    x_hbm, dy_hbm, gain_hbm, wg_hbm, wu_hbm, wd_hbm,
    dx_ref, dgain_ref, ddown_ref,
    x_ref, dy_ref, gain_ref, wg, wu, wd, xg, dyg, dyc, own_hid, hid, normed, d_in, d_out, d_pair, d_send, d_got, gz_own, gz, gg_own, gg,
    w_sem, x_s, x_r, xs_s, xs_r, y_s, y_r, ys_s, ys_r, cz_s, cz_r, c_s, c_r, cs_s, cs_r,
    h_s, h_r, p_s, p_r, d_s, d_r, gz_s, gz_r, gg_s, gg_r,
):
    r, f, t = lax.axis_index("rep"), lax.axis_index("fs"), lax.axis_index("tp")
    ng = 2 * nf
    me = 2 * f + t
    own, width = x_hbm.shape
    cols = ddown_ref.shape[1]
    sibling = (r, f, 1 - t)

    def chip(k):
        if nf & (nf - 1):
            return lax.rem(f + k + nf, nf)
        partner, bit = f, 1
        while bit < nf:
            if abs(k) & bit:
                partner = partner + bit - 2 * bit * lax.rem(partner // bit, 2)
            bit *= 2
        return partner

    def layer(k):
        return lax.rem(r + k + nr, nr)

    def member(k):
        g = lax.rem(me + k + ng, ng)
        return g, (r, g // 2, lax.rem(g, 2))

    def rows(g):
        return pl.ds(pl.multiple_of(g * own, own), own)

    def span(p):
        return pl.ds(pl.multiple_of(p * cols, LANES), cols)

    sent = []

    def send(src, dst, ssem, rsem, to):
        copy = pltpu.make_async_remote_copy(
            src_ref=src, dst_ref=dst, send_sem=ssem, recv_sem=rsem,
            device_id=to, device_id_type=MESH,
        )
        copy.start()
        sent.append(copy)

    def arrived(dst, ssem, rsem):
        pltpu.make_async_remote_copy(
            src_ref=dst, dst_ref=dst, send_sem=ssem, recv_sem=rsem,
            device_id=sibling, device_id_type=MESH,
        ).wait_recv()

    loads = [
        pltpu.make_async_copy(src, dst, w_sem.at[i])
        for i, (src, dst) in enumerate(
            (
                (x_hbm, x_ref), (dy_hbm, dy_ref), (gain_hbm, gain_ref),
                (wg_hbm, wg), (wu_hbm, wu), (wd_hbm, wd),
            )
        )
    ]
    for load in loads:
        load.start()

    barrier = pltpu.get_barrier_semaphore()
    for k in range(1, ng):
        pl.semaphore_signal(barrier, inc=1, device_id=member(k)[1], device_id_type=MESH)
    for k in range(1, nr):
        pl.semaphore_signal(barrier, inc=1, device_id=(layer(k), f, t), device_id_type=MESH)
    pl.semaphore_wait(barrier, ng - 1 + nr - 1)
    for load in loads[:3]:
        load.wait()

    for src, dst, ss, rs, bs, br in (
        (x_ref, xg, x_s, x_r, xs_s, xs_r), (dy_ref, dyg, y_s, y_r, ys_s, ys_r)
    ):
        for k in range(1, nf):
            send(src, dst.at[rows(me)], ss.at[k - 1], rs.at[k - 1], (r, chip(k), t))
        send(src, dst.at[rows(me)], bs.at[0], br.at[0], sibling)
    for k in range(1, nr):
        to = layer(k)
        send(
            dy_ref.at[:, span(to)], dyc.at[k - 1, rows(me)],
            cz_s.at[k - 1], cz_r.at[k - 1], (to, f, t),
        )
    xg[rows(me), :] = x_ref[...]
    dyg[rows(me), :] = dy_ref[...]

    def hand_on(ref, at, ss, rs, bs, br):
        for k in range(1, nf):
            block = at(ref, 2 * chip(-k) + t)
            arrived(block, ss.at[k - 1], rs.at[k - 1])
            send(block, block, bs.at[k], br.at[k], sibling)

    def from_sibling(ref, at, bs, br):
        for k in range(nf):
            arrived(at(ref, 2 * chip(-k) + 1 - t), bs.at[k], br.at[k])

    def plain(ref, g):
        return ref.at[rows(g)]

    def stacked(ref, g):
        return ref.at[:, rows(g)]

    hand_on(xg, plain, x_s, x_r, xs_s, xs_r)
    from_sibling(xg, plain, xs_s, xs_r)

    xf = xg[...].astype(jnp.float32)
    inv = lax.rsqrt(jnp.mean(xf * xf, axis=-1, keepdims=True) + EPS)
    normed[...] = xf * inv
    hidden_in = (normed[...] * gain_ref[...]).astype(jnp.bfloat16)
    for load in loads[3:]:
        load.wait()
    gate = across_columns(hidden_in, wg[...])
    up = across_columns(hidden_in, wu[...])

    sig = jax.nn.sigmoid(gate)
    act = gate * sig
    own_hid[...] = (act * up).astype(jnp.bfloat16)
    for k in range(1, nr):
        send(own_hid, hid.at[k - 1], h_s.at[k - 1], h_r.at[k - 1], (layer(k), f, t))

    hand_on(dyg, plain, y_s, y_r, ys_s, ys_r)
    for k in range(1, nr):
        arrived(dyc.at[k - 1, rows(me)], cz_s.at[k - 1], cz_r.at[k - 1])
    for k in range(1, nf):
        send(stacked(dyc, me), stacked(dyc, me), c_s.at[k - 1], c_r.at[k - 1], (r, chip(k), t))
    send(stacked(dyc, me), stacked(dyc, me), cs_s.at[0], cs_r.at[0], sibling)
    from_sibling(dyg, plain, ys_s, ys_r)
    d_hidden = 0.5 * across_columns(dyg[...], wd[...])
    d_gate = (d_hidden * up * sig * (1.0 + gate * (1.0 - sig))).astype(jnp.bfloat16)
    d_up = (d_hidden * act).astype(jnp.bfloat16)

    step = width // PIECES
    for p in range(PIECES):
        part = slice(p * step, (p + 1) * step)
        d_in[:, part] = jnp.dot(
            d_gate, wg[:, part], preferred_element_type=jnp.float32
        ) + jnp.dot(d_up, wu[:, part], preferred_element_type=jnp.float32)
        d_out[:, :, :, part] = (
            d_in[:, part].astype(jnp.bfloat16).reshape(nf, 2, own, step)
        )
        gg_own[:, part] = jnp.sum(d_in[:, part] * normed[:, part], axis=0, keepdims=True)
        send(
            d_out.at[:, 1 - t, :, part], d_pair.at[:, :, part], p_s.at[p], p_r.at[p], sibling
        )
    for k in range(1, ng):
        send(gg_own, gg.at[me], gg_s.at[k - 1], gg_r.at[k - 1], member(k)[1])
    gg[me] = gg_own[...]

    for p in range(PIECES):
        part = slice(p * step, (p + 1) * step)
        arrived(d_pair.at[:, :, part], p_s.at[p], p_r.at[p])
        for k in range(1, nf):
            to = chip(k)
            d_send[k - 1, :, part] = (
                d_in[rows(2 * to + t), part] + d_pair[to, :, part].astype(jnp.float32)
            ).astype(jnp.bfloat16)
            send(
                d_send.at[k - 1, :, part], d_got.at[k - 1, :, part],
                d_s.at[p, k - 1], d_r.at[p, k - 1], (r, to, t),
            )

    hand_on(dyc, stacked, c_s, c_r, cs_s, cs_r)
    for k in range(1, ng):
        arrived(gg.at[member(-k)[0]], gg_s.at[k - 1], gg_r.at[k - 1])
    gz_own[...] = jnp.sum(gg[...], axis=0)
    for k in range(1, nr):
        send(gz_own, gz.at[r], gz_s.at[k - 1], gz_r.at[k - 1], (layer(k), f, t))
    gz[r] = gz_own[...]
    total = across_tokens(own_hid[...], dyg[:, span(r)])

    mine = d_in[rows(me), :] + d_pair[f].astype(jnp.float32)
    for k in range(1, nf):
        for p in range(PIECES):
            arrived(
                d_got.at[k - 1, :, slice(p * step, (p + 1) * step)],
                d_s.at[p, k - 1], d_r.at[p, k - 1],
            )
        mine = mine + d_got[k - 1].astype(jnp.float32)
    xf = x_ref[...].astype(jnp.float32)
    own_inv = lax.rsqrt(jnp.mean(xf * xf, axis=-1, keepdims=True) + EPS)
    own_normed = xf * own_inv
    scaled = mine * gain_ref[...]
    dx_ref[...] = (
        own_inv * (scaled - own_normed * jnp.mean(scaled * own_normed, axis=-1, keepdims=True))
    ).astype(jnp.bfloat16)

    from_sibling(dyc, stacked, cs_s, cs_r)
    for k in range(1, nr):
        arrived(hid.at[k - 1], h_s.at[k - 1], h_r.at[k - 1])
        total = total + across_tokens(hid[k - 1], dyc[k - 1])
    ddown_ref[...] = 0.5 * total

    for k in range(1, nr):
        arrived(gz.at[layer(-k)], gz_s.at[k - 1], gz_r.at[k - 1])
    dgain_ref[...] = jnp.sum(gz[...], axis=0)
    for copy in sent:
        copy.wait_send()


def put(a, b, c, a_out, b_out, c_out, sem):
    copies = [
        pltpu.make_async_copy(src, dst, sem.at[i])
        for i, (src, dst) in enumerate(((a, a_out), (b, b_out), (c, c_out)))
    ]
    for copy in copies:
        copy.start()
    for copy in copies:
        copy.wait()


def fused(nr, nf, inputs, cotangent, norm_gain, gate_weight, up_weight, down_weight):
    own, width = inputs.shape
    share = gate_weight.shape[1]
    ng = 2 * nf
    group, cols = ng * own, width // nr
    bf16, f32 = jnp.bfloat16, jnp.float32
    vmem = pl.BlockSpec(memory_space=pltpu.VMEM)
    hbm = pl.BlockSpec(memory_space=pltpu.HBM)
    dma = pltpu.SemaphoreType.DMA
    pair = lambda *n: [dma(n), dma(n)]
    results = pl.pallas_call(
        functools.partial(kernel, nr, nf),
        out_shape=(
            jax.ShapeDtypeStruct((own, width), bf16),
            jax.ShapeDtypeStruct((1, width), f32),
            jax.ShapeDtypeStruct((share, cols), f32),
        ),
        in_specs=[hbm] * 6,
        out_specs=(vmem,) * 3,
        scratch_shapes=[
            pltpu.VMEM((own, width), bf16),
            pltpu.VMEM((own, width), bf16),
            pltpu.VMEM((1, width), f32),
            pltpu.VMEM((share, width), bf16),
            pltpu.VMEM((share, width), bf16),
            pltpu.VMEM((share, width), bf16),
            pltpu.VMEM((group, width), bf16),
            pltpu.VMEM((group, width), bf16),
            pltpu.VMEM((nr - 1, group, cols), bf16),
            pltpu.VMEM((group, share), bf16),
            pltpu.VMEM((nr - 1, group, share), bf16),
            pltpu.VMEM((group, width), f32),
            pltpu.VMEM((group, width), f32),
            pltpu.VMEM((nf, 2, own, width), bf16),
            pltpu.VMEM((nf, own, width), bf16),
            pltpu.VMEM((nf - 1, own, width), bf16),
            pltpu.VMEM((nf - 1, own, width), bf16),
            pltpu.VMEM((1, width), f32),
            pltpu.VMEM((nr, 1, width), f32),
            pltpu.VMEM((1, width), f32),
            pltpu.VMEM((ng, 1, width), f32),
            dma((6,)),
        ]
        + pair(nf - 1) + pair(nf) + pair(nf - 1) + pair(nf)
        + pair(nr - 1) + pair(nf - 1) + pair(nf)
        + pair(nr - 1) + pair(PIECES) + pair(PIECES, nf - 1) + pair(nr - 1) + pair(ng - 1),
        compiler_params=pltpu.CompilerParams(
            collective_id=0, has_side_effects=True, vmem_limit_bytes=52 * 1024 * 1024
        ),
    )(*[
        pltpu.with_memory_space_constraint(a, pltpu.HBM)
        for a in (
            inputs, cotangent, norm_gain[None], gate_weight.T, up_weight.T, down_weight
        )
    ])
    dx, dgain, ddown = pl.pallas_call(
        put,
        out_shape=tuple(jax.ShapeDtypeStruct(a.shape, a.dtype) for a in results),
        in_specs=[vmem] * 3,
        out_specs=(hbm,) * 3,
        scratch_shapes=[dma((3,))],
        compiler_params=pltpu.CompilerParams(vmem_limit_bytes=52 * 1024 * 1024),
    )(*results)
    return dx, dgain[0], ddown


def solution(mesh):
    nr, nf, nt = (mesh.shape[name] for name in ("rep", "fs", "tp"))

    def body(inputs, *others):
        block = inputs.shape[1] // nr
        if nt == 2 and nr > 1 and nf > 1 and block % LANES == 0 and inputs.shape[0] % 16 == 0:
            return fused(nr, nf, inputs, *others)
        return per_device(inputs, *others)

    return jax.shard_map(
        body,
        mesh=mesh,
        in_specs=(
            P(("rep", "fs", "tp"), None),
            P(("rep", "fs", "tp"), None),
            P(),
            P(None, ("fs", "tp")),
            P(None, ("fs", "tp")),
            P(("fs", "tp"), None),
        ),
        out_specs=(P(("rep", "fs", "tp"), None), P(), P(("fs", "tp"), "rep")),
        check_vma=False,
    )
```
